32 devices in a mesh: sp: 8 (over z, y), dp: 4 (over x, core).
Axes of the slice: x: 2, y: 2, z: 4, core: 2. Of those that a mesh axis runs over, the one named last changes fastest.
Arguments:
- queries: bfloat16 [4, 2048, 1280], P('dp', None, 'sp'), may hold values from -6 to 6
- keys: bfloat16 [4, 1024, 1280], P('dp', None, 'sp'), may hold values from -6 to 6
- values: bfloat16 [4, 1024, 1280], P('dp', None, 'sp'), may hold values from -48 to 48
- q_gain: float32 [64], replicated, may hold values from 0.5 to 10
- k_gain: float32 [64], replicated, may hold values from 0.5 to 10
- w_out: bfloat16 [2048, 2048], P(None, 'dp'), may hold values from -0.125 to 0.125
Outputs:
- mixed: bfloat16 [4, 1280, 2048], P('dp', 'sp')
The draws below stay inside these ranges and needn't reach their ends.
All inputs are finite; a program needn't handle non-finite values.
Results may differ from the reference program's by a relative error of at most 0.0038.
The reference program's roundings to bfloat16 on the way count: a program that leaves them out, or rounds other values in their place, can miss the bound.
Values may be sent and summed in bfloat16 or wider, within the bound.
A program may use at most 64 MiB of HBM per device.

```python
import jax
import jax.numpy as jnp
from jax import lax

HD = 64
QH = 32
KV = 16
D = 2048
GRID_W = 64
QW = 2048
KVW = 1024
TOKENS = 1280
SEQ_GROUPS = 4


def shared_keys(key):
    key_draw = jax.random.normal(jax.random.fold_in(key, 11), (SEQ_GROUPS, KVW, TOKENS), jnp.float32)
    return jnp.clip(key_draw, -6.0, 6.0)


def draw_keys(key, part):
    return shared_keys(key).astype(jnp.bfloat16)


def draw_queries(key, part):
    fresh_draw = jax.random.normal(jax.random.fold_in(key, 12), (SEQ_GROUPS, QW, TOKENS), jnp.float32)
    fresh_draw = jnp.clip(fresh_draw, -6.0, 6.0)
    return fresh_draw.astype(jnp.bfloat16)


def gain_draw(key, salt):
    noise_draw = jnp.clip(jax.random.normal(jax.random.fold_in(key, salt), (HD,), jnp.float32), -3.0, 3.0)
    return 1.25 * (1.0 + 0.18 * noise_draw)


def draw_q_gain(key, part):
    return gain_draw(key, 21)


def draw_k_gain(key, part):
    return gain_draw(key, 22)


def steps_of(rng, dims, split, least, top_value):
    level = 1.0
    for axis_at, parts in split:
        draws = jax.random.uniform(jax.random.fold_in(jax.random.fold_in(rng, 6), axis_at), (parts,), jnp.float32, least / len(split), top_value / len(split))
        level = level * jnp.repeat(jnp.exp(draws), dims[axis_at] // parts).reshape((-1,) + (1,) * (len(dims) - 1 - axis_at))
    return level


def noise(rng, shape, spread, reach, split=(), held_as=jnp.bfloat16):
    result = jax.random.normal(rng, shape, jnp.float32) * spread
    if len(split) > 0:
        result = steps_of(rng, shape, split, -0.22, 0.18) * result
    return jnp.clip(result, min=-reach, max=reach).astype(held_as)


def setup_inputs(seed: int = 0) -> dict:
    key_list = jax.random.split(jax.random.key(seed), 7)
    queries = draw_queries(jax.random.fold_in(key_list[6], 71), 0)
    keys = draw_keys(jax.random.fold_in(key_list[6], 71), 0)
    values = noise(key_list[2], (SEQ_GROUPS, KVW, TOKENS), 8.0, 48.0, ((0, 4), (2, 8)))
    q_gain = draw_q_gain(jax.random.fold_in(key_list[6], 71), 0)
    k_gain = draw_k_gain(jax.random.fold_in(key_list[6], 71), 0)
    w_out = noise(key_list[5], (QW, D), QW ** -0.5, 0.125, ((1, 4),))
    return dict(queries=queries, keys=keys, values=values, q_gain=q_gain, k_gain=k_gain, w_out=w_out)


epsilon = 1e-06
rotary_base = 10000.0

def rotary_tables(row_count):
    position = jnp.arange(row_count, dtype=jnp.int32)
    grid_row = (position // GRID_W).astype(jnp.float32)
    grid_col = (position % GRID_W).astype(jnp.float32)
    quarter = HD // 4
    inv_freq = rotary_base ** (-(2.0 * jnp.arange(quarter, dtype=jnp.float32)) / (HD // 2))
    row_angle = inv_freq[:, None] * grid_row[None, :]
    col_angle = inv_freq[:, None] * grid_col[None, :]
    cos_table = jnp.concatenate([jnp.cos(row_angle), jnp.cos(row_angle), jnp.cos(col_angle), jnp.cos(col_angle)], axis=0)
    sin_table = jnp.concatenate([jnp.sin(row_angle), jnp.sin(row_angle), jnp.sin(col_angle), jnp.sin(col_angle)], axis=0)
    return (cos_table, sin_table)

def normalize_turn(field, gain, cos_table, sin_table):
    head_count = field.shape[0] // HD
    values_f = field.astype(jnp.float32).reshape(head_count, HD, field.shape[1])
    normed = values_f * lax.rsqrt(lax.optimization_barrier(jnp.mean(values_f * values_f, axis=1, keepdims=True)) + epsilon) * gain[None, :, None]
    quarter = HD // 4
    quarters_of = normed.reshape(head_count, 4, quarter, field.shape[1])
    turned = jnp.concatenate([-quarters_of[:, 1], quarters_of[:, 0], -quarters_of[:, 3], quarters_of[:, 2]], axis=1)
    return (normed * cos_table[None] + turned * sin_table[None]).astype(jnp.bfloat16)

def reference(queries, keys, values, q_gain, k_gain, w_out):
    cos_table, sin_table = rotary_tables(TOKENS)
    group_size = QH // KV
    score_scale = HD ** (-0.5)

    def per_group(packed):
        query_rows, key_rows, value_rows = packed
        query_rot = normalize_turn(query_rows, q_gain, cos_table, sin_table)
        key_rot = normalize_turn(key_rows, k_gain, cos_table, sin_table)
        value_heads = value_rows.reshape(KV, HD, TOKENS)

        def per_head(head_index):
            query_one = lax.dynamic_index_in_dim(query_rot, head_index, 0, keepdims=False)
            key_one = lax.dynamic_index_in_dim(key_rot, head_index // group_size, 0, keepdims=False)
            value_one = lax.dynamic_index_in_dim(value_heads, head_index // group_size, 0, keepdims=False)
            scores = jnp.einsum('dq,dk->qk', query_one.astype(jnp.float32), key_one.astype(jnp.float32)) * score_scale
            row_max = lax.optimization_barrier(jnp.max(scores, axis=-1, keepdims=True))
            weights = jnp.exp(scores - row_max)
            weights = (weights / lax.optimization_barrier(jnp.sum(weights, axis=-1, keepdims=True))).astype(jnp.bfloat16)
            attended = jnp.einsum('qk,dk->dq', weights.astype(jnp.float32), value_one.astype(jnp.float32))
            return attended.astype(jnp.bfloat16)
        attended = lax.map(per_head, jnp.arange(QH, dtype=jnp.int32)).reshape(QW, TOKENS)
        return jnp.dot(attended.T, w_out, preferred_element_type=jnp.float32).astype(jnp.bfloat16)
    return lax.map(per_group, (queries, keys, values))
```

```python
import functools

import jax
import jax.numpy as jnp
from jax import lax
from jax.experimental import pallas as pl
from jax.experimental.pallas import tpu as pltpu
from jax.sharding import PartitionSpec as P

HD = 64
QH = 32
KV = 16
GRID_W = 64


epsilon = 1e-06
rotary_base = 10000.0
block_count = 8


def swapped(block, axis, apart):
    count = lax.axis_size(axis)
    route = []
    for low in range(count):
        high = low | 1 << apart
        if high != low and high < count:
            route += [(low, high), (high, low)]
    return lax.ppermute(block, axis, route)


def rotary_tables(first_row, row_count):
    position = first_row + lax.iota(jnp.int32, row_count)
    grid_row = (position // GRID_W).astype(jnp.float32)
    grid_col = (position % GRID_W).astype(jnp.float32)
    quarter = HD // 4
    inv_freq = rotary_base ** (-(2.0 * lax.iota(jnp.float32, quarter)) / (HD // 2))
    row_angle = inv_freq[:, None] * grid_row[None, :]
    col_angle = inv_freq[:, None] * grid_col[None, :]
    cos_table = jnp.concatenate(
        [jnp.cos(row_angle), jnp.cos(row_angle), jnp.cos(col_angle), jnp.cos(col_angle)], axis=0
    )
    sin_table = jnp.concatenate(
        [jnp.sin(row_angle), jnp.sin(row_angle), jnp.sin(col_angle), jnp.sin(col_angle)], axis=0
    )
    return (cos_table, sin_table)


def normalize_turn(field, gain, cos_table, sin_table):
    head_count = field.shape[0] // HD
    values_f = field.astype(jnp.float32).reshape(head_count, HD, field.shape[1])
    normed = (
        values_f
        * lax.rsqrt(jnp.mean(values_f * values_f, axis=1, keepdims=True) + epsilon)
        * gain[None, :, None]
    )
    quarter = HD // 4
    quarters_of = normed.reshape(head_count, 4, quarter, field.shape[1])
    turned = jnp.concatenate(
        [-quarters_of[:, 1], quarters_of[:, 0], -quarters_of[:, 3], quarters_of[:, 2]], axis=1
    )
    return (normed * cos_table[None] + turned * sin_table[None]).astype(jnp.bfloat16)


def attention_heads(query_heads, key_heads, value_heads, seq_len):
    kv_local = key_heads.shape[0]
    group_local = query_heads.shape[0] // kv_local
    query_split = query_heads.reshape(kv_local, group_local, HD, seq_len)
    score_scale = HD ** (-0.5)
    block_rows = seq_len // block_count

    def one_block(block_index, result):
        row_start = block_index * block_rows
        query_block = lax.dynamic_slice_in_dim(query_split, row_start, block_rows, 3)
        scores = (
            jnp.einsum("hgdq,hdk->hgqk", query_block, key_heads, preferred_element_type=jnp.float32)
            * score_scale
        )
        row_max = jnp.max(scores, axis=-1, keepdims=True)
        weights = jnp.exp(scores - row_max)
        weights = (weights / jnp.sum(weights, axis=-1, keepdims=True)).astype(jnp.bfloat16)
        attended = jnp.einsum(
            "hgqk,hdk->hgdq", weights, value_heads, preferred_element_type=jnp.float32
        )
        return lax.dynamic_update_slice_in_dim(result, attended.astype(jnp.bfloat16), row_start, 3)

    result = jnp.zeros(query_split.shape, jnp.bfloat16)
    result = lax.fori_loop(0, block_count, one_block, result)
    return result.reshape(query_heads.shape)


def on_device_plain(queries, keys, values, q_gain, k_gain, w_out):
    sp_count = lax.axis_size("sp")
    tok_rows = queries.shape[2]
    seq_len = tok_rows * sp_count
    cos_table, sin_table = rotary_tables(lax.axis_index("sp") * tok_rows, tok_rows)
    query_rot = normalize_turn(queries[0], q_gain, cos_table, sin_table)
    key_rot = normalize_turn(keys[0], k_gain, cos_table, sin_table)
    value_rows = values[0].reshape(KV, HD, tok_rows)
    query_heads = lax.all_to_all(query_rot, "sp", split_axis=0, concat_axis=2, tiled=True)
    share_count = max(sp_count // KV, 1)
    part_rows = tok_rows // share_count
    key_cut = (
        key_rot.reshape(KV, HD, share_count, part_rows)
        .transpose(0, 2, 1, 3)
        .reshape(KV * share_count, HD, part_rows)
    )
    value_cut = (
        value_rows.reshape(KV, HD, share_count, part_rows)
        .transpose(0, 2, 1, 3)
        .reshape(KV * share_count, HD, part_rows)
    )
    key_got, value_got = (
        lax.all_to_all(key_cut, "sp", split_axis=0, concat_axis=2, tiled=True),
        lax.all_to_all(value_cut, "sp", split_axis=0, concat_axis=2, tiled=True),
    )
    kv_local = key_got.shape[0]
    key_got = key_got.reshape(kv_local, HD, sp_count, part_rows)
    value_got = value_got.reshape(kv_local, HD, sp_count, part_rows)
    for bit_index in range(share_count.bit_length() - 1):
        key_other, value_other = swapped((key_got, value_got), "sp", bit_index)
        key_got = jnp.concatenate([key_got, key_other], axis=3)
        value_got = jnp.concatenate([value_got, value_other], axis=3)
    key_heads = key_got.reshape(kv_local, HD, seq_len)
    value_heads = value_got.reshape(kv_local, HD, seq_len)
    attended = attention_heads(query_heads, key_heads, value_heads, seq_len)
    token_heads = lax.all_to_all(attended, "sp", split_axis=2, concat_axis=0, tiled=True)
    token_rows = token_heads.reshape(QH * HD, tok_rows)
    product = lax.dot_general(
        token_rows,
        lax.all_gather(w_out, "dp", axis=1, tiled=True),
        (((0,), (0,)), ((), ())),
        preferred_element_type=jnp.float32,
    )
    mixed_rows = product.astype(jnp.bfloat16)
    return mixed_rows[None]


MESH = pl.DeviceIdType.MESH
LOG2E = 1.4426950408889634


def layer_kernel(
    n, m, q_ref, k_ref, v_ref, qg_ref, kg_ref, cos_ref, sin_ref, w_ref, out_ref,
    q_out, k_out, v_out, q_in, k_in, v_in, a_out, a_in, w_all,
    q_send, q_recv, k_send, k_recv, v_send, v_recv, a_send, a_recv, w_send, w_recv, w_pass, w_own,
):
    me = lax.axis_index("sp")
    dp = lax.axis_index("dp")
    x_count = m // 2
    core = lax.rem(dp, 2)
    x_at = dp // 2
    partner = x_at * 2 + (1 - core)
    rows = q_ref.shape[1]
    w_rows = w_ref.shape[0] // n
    kv_width = k_out.shape[2]
    pairs = kv_width // 128
    group = q_out.shape[2] // kv_width

    def at_sp(d):
        return lax.rem(me + d, n)

    def at_dp(d):
        return lax.rem(x_at + d, x_count) * 2 + core

    barrier = pltpu.get_barrier_semaphore()

    def greet(d, carry):
        pl.semaphore_signal(barrier, inc=1, device_id={"sp": at_sp(d)}, device_id_type=MESH)
        return carry

    lax.fori_loop(1, n, greet, 0)
    for d in range(1, x_count):
        pl.semaphore_signal(barrier, inc=1, device_id={"dp": at_dp(d)}, device_id_type=MESH)
    pl.semaphore_signal(barrier, inc=1, device_id={"dp": partner}, device_id_type=MESH)
    pl.semaphore_wait(barrier, n - 1 + x_count)

    def w_piece(shard, c):
        return w_all.at[shard, pl.ds(pl.multiple_of(c * w_rows, w_rows), w_rows)]

    def w_source(c):
        return w_ref.at[pl.ds(pl.multiple_of(c * w_rows, w_rows), w_rows)]

    def w_copy(d, c):
        return pltpu.make_async_remote_copy(
            src_ref=w_source(c), dst_ref=w_piece(dp, c), send_sem=w_send.at[d, c],
            recv_sem=w_recv.at[dp, c], device_id={"dp": at_dp(d) if d else partner},
            device_id_type=MESH,
        )

    def w_came(shard, c):
        return pltpu.make_async_remote_copy(
            src_ref=w_source(c), dst_ref=w_piece(shard, c), send_sem=w_send.at[0, c],
            recv_sem=w_recv.at[shard, c], device_id={"dp": partner}, device_id_type=MESH,
        )

    def w_forward(d, c):
        shard = at_dp(d)
        return pltpu.make_async_remote_copy(
            src_ref=w_piece(shard, c), dst_ref=w_piece(shard, c), send_sem=w_pass.at[d, c],
            recv_sem=w_recv.at[shard, c], device_id={"dp": partner}, device_id_type=MESH,
        )

    def start_w(c, carry):
        for d in range(x_count):
            w_copy(d, c).start()
        return carry

    lax.fori_loop(0, n, start_w, 0)
    own_w = pltpu.make_async_copy(w_ref, w_all.at[dp], w_own)
    own_w.start()

    eye = jnp.where(
        lax.broadcasted_iota(jnp.int32, (rows, rows), 0)
        == lax.broadcasted_iota(jnp.int32, (rows, rows), 1), 1.0, 0.0,
    ).astype(jnp.bfloat16)

    def flip(block):
        return lax.dot_general(
            eye, block, (((1,), (1,)), ((), ())), preferred_element_type=jnp.float32
        ).astype(jnp.bfloat16)

    def turn(block, gain):
        u = block.astype(jnp.float32)
        normed = u * lax.rsqrt(jnp.mean(u * u, axis=0, keepdims=True) + epsilon) * gain
        part = HD // 4
        a, b, c, d = (normed[i * part : (i + 1) * part] for i in range(4))
        turned = jnp.concatenate([-b, a, -d, c], axis=0)
        return (normed * cos_ref[...] + turned * sin_ref[...]).astype(jnp.bfloat16)

    def exchange(out, into, send, recv, d):
        peer = at_sp(d)
        return pltpu.make_async_remote_copy(
            src_ref=out.at[peer], dst_ref=into.at[me], send_sem=send.at[peer],
            recv_sem=recv.at[me], device_id={"sp": peer}, device_id_type=MESH,
        )

    def arrival(out, into, send, recv, source):
        return pltpu.make_async_remote_copy(
            src_ref=out.at[source], dst_ref=into.at[source], send_sem=send.at[source],
            recv_sem=recv.at[source], device_id={"sp": source}, device_id_type=MESH,
        )

    def kv_heads_of(peer):
        base = pl.multiple_of(peer * kv_width, kv_width)
        kt = jnp.concatenate(
            [turn(k_ref[pl.ds(base + h * HD, HD)], kg_ref[...]) for h in range(kv_width // HD)], axis=0
        )
        return flip(kt), flip(v_ref[pl.ds(base, kv_width)])

    def q_heads_of(peer):
        base = pl.multiple_of(peer * (kv_width * group), kv_width * group)
        parts = []
        for g in range(group):
            for h in range(kv_width // HD):
                parts.append(turn(q_ref[pl.ds(base + (h * group + g) * HD, HD)], qg_ref[...]))
        return flip(jnp.concatenate(parts, axis=0))

    def send_kv(d, carry):
        peer = at_sp(d)
        k_out[peer], v_out[peer] = kv_heads_of(peer)
        exchange(k_out, k_in, k_send, k_recv, d).start()
        exchange(v_out, v_in, v_send, v_recv, d).start()
        return carry

    def send_q(d, carry):
        peer = at_sp(d)
        q_out[peer] = q_heads_of(peer)
        exchange(q_out, q_in, q_send, q_recv, d).start()
        return carry

    lax.fori_loop(1, n, send_kv, 0)
    lax.fori_loop(1, n, send_q, 0)
    k_in[me], v_in[me] = kv_heads_of(me)
    q_in[me] = q_heads_of(me)

    def await_kv(d, carry):
        source = at_sp(d)
        arrival(k_out, k_in, k_send, k_recv, source).wait_recv()
        arrival(v_out, v_in, v_send, v_recv, source).wait_recv()
        return carry

    lax.fori_loop(1, n, await_kv, 0)
    seq_len = n * rows
    low = lax.broadcasted_iota(jnp.int32, (rows, 128), 1) < HD
    scale = HD ** (-0.5) * LOG2E

    def attend(source):
        for j in range(pairs):
            keys = k_in[:, :, j * 128 : (j + 1) * 128].reshape(seq_len, 128)
            vals = v_in[:, :, j * 128 : (j + 1) * 128].reshape(seq_len, 128)
            tiles = []
            for g in range(group):
                at = g * kv_width + j * 128
                pair = q_in[source, :, at : at + 128]
                zero = jnp.zeros_like(pair)
                both = []
                for one in (jnp.where(low, pair, zero), jnp.where(low, zero, pair)):
                    s = lax.dot_general(
                        one, keys, (((1,), (1,)), ((), ())), preferred_element_type=jnp.float32
                    )
                    p = jnp.exp2((s - jnp.max(s, axis=1, keepdims=True)) * scale)
                    p = p * (1.0 / jnp.sum(p, axis=1, keepdims=True))
                    both.append(
                        jnp.dot(p.astype(jnp.bfloat16), vals, preferred_element_type=jnp.float32)
                    )
                tiles.append(jnp.where(low, both[0], both[1]))
            first, second = tiles
            one = jnp.where(low, first, pltpu.roll(second, HD, 1))
            two = jnp.where(low, pltpu.roll(first, HD, 1), second)
            yield j, jnp.concatenate([one, two], axis=1).astype(jnp.bfloat16)

    def block(d, carry):
        source = at_sp(d)
        arrival(q_out, q_in, q_send, q_recv, source).wait_recv()
        for j, tile in attend(source):
            a_out[source, :, j * 256 : (j + 1) * 256] = tile
        exchange(a_out, a_in, a_send, a_recv, d).start()
        for e in range(1, x_count):
            w_came(at_dp(e), d - 1).wait_recv()
            w_forward(e, d - 1).start()
        return carry

    lax.fori_loop(1, n, block, 0)
    for j, tile in attend(me):
        a_in[me, :, j * 256 : (j + 1) * 256] = tile
    own_w.wait()

    def came(d, carry):
        source = at_sp(d)
        arrival(a_out, a_in, a_send, a_recv, source).wait_recv()
        return carry

    lax.fori_loop(1, n, came, 0)
    width = w_ref.shape[1]

    def product(shard):
        total = jnp.zeros((rows, width), jnp.float32)
        step = a_in.shape[2]
        for p in range(n):
            total += jnp.dot(
                a_in[p], w_all[shard, p * step : (p + 1) * step, :],
                preferred_element_type=jnp.float32,
            )
        out_ref[:, pl.ds(pl.multiple_of(shard * width, width), width)] = total.astype(jnp.bfloat16)

    def await_w(shard):
        def one(c, carry):
            w_came(shard, c).wait_recv()
            return carry

        lax.fori_loop(0, n, one, 0)

    product(dp)
    await_w(partner)
    product(partner)
    for e in range(1, x_count):
        w_came(at_dp(e), n - 1).wait_recv()
        w_forward(e, n - 1).start()
    for e in range(1, x_count):
        product(at_dp(e))
    for e in range(1, x_count):
        other = at_dp(e) + 1 - 2 * core
        await_w(other)
        product(other)

    def sent(d, carry):
        exchange(k_out, k_in, k_send, k_recv, d).wait_send()
        exchange(v_out, v_in, v_send, v_recv, d).wait_send()
        exchange(q_out, q_in, q_send, q_recv, d).wait_send()
        exchange(a_out, a_in, a_send, a_recv, d).wait_send()
        return carry

    lax.fori_loop(1, n, sent, 0)

    def sent_w(c, carry):
        for d in range(x_count):
            w_copy(d, c).wait_send()
        for d in range(1, x_count):
            w_forward(d, c).wait_send()
        return carry

    lax.fori_loop(0, n, sent_w, 0)


def on_device(queries, keys, values, q_gain, k_gain, w_out):
    n, m = lax.axis_size("sp"), lax.axis_size("dp")
    tok_rows = queries.shape[2]
    kv_width = keys.shape[1] // n
    if kv_width % 128 or m % 2 or tok_rows % 16:
        return on_device_plain(queries, keys, values, q_gain, k_gain, w_out)
    q_width = queries.shape[1] // n
    cos_table, sin_table = rotary_tables(lax.axis_index("sp") * tok_rows, tok_rows)
    vmem = pl.BlockSpec(memory_space=pltpu.VMEM)
    bf16 = jnp.bfloat16
    dma = pltpu.SemaphoreType.DMA
    mixed = pl.pallas_call(
        functools.partial(layer_kernel, n, m),
        out_shape=jax.ShapeDtypeStruct((tok_rows, w_out.shape[1] * m), bf16),
        in_specs=[vmem] * 7 + [pl.BlockSpec(memory_space=pl.ANY)],
        out_specs=vmem,
        scratch_shapes=[
            pltpu.VMEM((n, tok_rows, q_width), bf16),
            pltpu.VMEM((n, tok_rows, kv_width), bf16),
            pltpu.VMEM((n, tok_rows, kv_width), bf16),
            pltpu.VMEM((n, tok_rows, q_width), bf16),
            pltpu.VMEM((n, tok_rows, kv_width), bf16),
            pltpu.VMEM((n, tok_rows, kv_width), bf16),
            pltpu.VMEM((n, tok_rows, q_width), bf16),
            pltpu.VMEM((n, tok_rows, q_width), bf16),
            pltpu.VMEM((m, w_out.shape[0], w_out.shape[1]), bf16),
        ]
        + [dma((n,))] * 8
        + [dma((m // 2, n)), dma((m, n)), dma((m // 2, n)), dma],
        compiler_params=pltpu.CompilerParams(
            collective_id=0, has_side_effects=True, vmem_limit_bytes=48 * 1024 * 1024
        ),
    )(
        queries[0], keys[0], values[0], q_gain[:, None], k_gain[:, None],
        cos_table, sin_table, w_out,
    )
    return mixed[None]


def solution(mesh):
    placed = (
        P("dp", None, "sp"),
        P("dp", None, "sp"),
        P("dp", None, "sp"),
        P(),
        P(),
        P(None, "dp"),
    )
    return jax.shard_map(
        on_device, mesh=mesh, in_specs=placed, out_specs=P("dp", "sp", None), check_vma=False
    )
```

```python
import functools

import jax
import jax.numpy as jnp
from jax import lax
from jax.experimental import pallas as pl
from jax.experimental.pallas import tpu as pltpu
from jax.sharding import PartitionSpec as P

HD = 64
QH = 32
KV = 16
GRID_W = 64


epsilon = 1e-06
rotary_base = 10000.0
block_count = 8


def swapped(block, axis, apart):
    count = lax.axis_size(axis)
    route = []
    for low in range(count):
        high = low | 1 << apart
        if high != low and high < count:
            route += [(low, high), (high, low)]
    return lax.ppermute(block, axis, route)


def rotary_tables(first_row, row_count):
    position = first_row + lax.iota(jnp.int32, row_count)
    grid_row = (position // GRID_W).astype(jnp.float32)
    grid_col = (position % GRID_W).astype(jnp.float32)
    quarter = HD // 4
    inv_freq = rotary_base ** (-(2.0 * lax.iota(jnp.float32, quarter)) / (HD // 2))
    row_angle = inv_freq[:, None] * grid_row[None, :]
    col_angle = inv_freq[:, None] * grid_col[None, :]
    cos_table = jnp.concatenate(
        [jnp.cos(row_angle), jnp.cos(row_angle), jnp.cos(col_angle), jnp.cos(col_angle)], axis=0
    )
    sin_table = jnp.concatenate(
        [jnp.sin(row_angle), jnp.sin(row_angle), jnp.sin(col_angle), jnp.sin(col_angle)], axis=0
    )
    return (cos_table, sin_table)


def normalize_turn(field, gain, cos_table, sin_table):
    head_count = field.shape[0] // HD
    values_f = field.astype(jnp.float32).reshape(head_count, HD, field.shape[1])
    normed = (
        values_f
        * lax.rsqrt(jnp.mean(values_f * values_f, axis=1, keepdims=True) + epsilon)
        * gain[None, :, None]
    )
    quarter = HD // 4
    quarters_of = normed.reshape(head_count, 4, quarter, field.shape[1])
    turned = jnp.concatenate(
        [-quarters_of[:, 1], quarters_of[:, 0], -quarters_of[:, 3], quarters_of[:, 2]], axis=1
    )
    return (normed * cos_table[None] + turned * sin_table[None]).astype(jnp.bfloat16)


def attention_heads(query_heads, key_heads, value_heads, seq_len):
    kv_local = key_heads.shape[0]
    group_local = query_heads.shape[0] // kv_local
    query_split = query_heads.reshape(kv_local, group_local, HD, seq_len)
    score_scale = HD ** (-0.5)
    block_rows = seq_len // block_count

    def one_block(block_index, result):
        row_start = block_index * block_rows
        query_block = lax.dynamic_slice_in_dim(query_split, row_start, block_rows, 3)
        scores = (
            jnp.einsum("hgdq,hdk->hgqk", query_block, key_heads, preferred_element_type=jnp.float32)
            * score_scale
        )
        row_max = jnp.max(scores, axis=-1, keepdims=True)
        weights = jnp.exp(scores - row_max)
        weights = (weights / jnp.sum(weights, axis=-1, keepdims=True)).astype(jnp.bfloat16)
        attended = jnp.einsum(
            "hgqk,hdk->hgdq", weights, value_heads, preferred_element_type=jnp.float32
        )
        return lax.dynamic_update_slice_in_dim(result, attended.astype(jnp.bfloat16), row_start, 3)

    result = jnp.zeros(query_split.shape, jnp.bfloat16)
    result = lax.fori_loop(0, block_count, one_block, result)
    return result.reshape(query_heads.shape)


def on_device_plain(queries, keys, values, q_gain, k_gain, w_out):
    sp_count = lax.axis_size("sp")
    tok_rows = queries.shape[2]
    seq_len = tok_rows * sp_count
    cos_table, sin_table = rotary_tables(lax.axis_index("sp") * tok_rows, tok_rows)
    query_rot = normalize_turn(queries[0], q_gain, cos_table, sin_table)
    key_rot = normalize_turn(keys[0], k_gain, cos_table, sin_table)
    value_rows = values[0].reshape(KV, HD, tok_rows)
    query_heads = lax.all_to_all(query_rot, "sp", split_axis=0, concat_axis=2, tiled=True)
    share_count = max(sp_count // KV, 1)
    part_rows = tok_rows // share_count
    key_cut = (
        key_rot.reshape(KV, HD, share_count, part_rows)
        .transpose(0, 2, 1, 3)
        .reshape(KV * share_count, HD, part_rows)
    )
    value_cut = (
        value_rows.reshape(KV, HD, share_count, part_rows)
        .transpose(0, 2, 1, 3)
        .reshape(KV * share_count, HD, part_rows)
    )
    key_got, value_got = (
        lax.all_to_all(key_cut, "sp", split_axis=0, concat_axis=2, tiled=True),
        lax.all_to_all(value_cut, "sp", split_axis=0, concat_axis=2, tiled=True),
    )
    kv_local = key_got.shape[0]
    key_got = key_got.reshape(kv_local, HD, sp_count, part_rows)
    value_got = value_got.reshape(kv_local, HD, sp_count, part_rows)
    for bit_index in range(share_count.bit_length() - 1):
        key_other, value_other = swapped((key_got, value_got), "sp", bit_index)
        key_got = jnp.concatenate([key_got, key_other], axis=3)
        value_got = jnp.concatenate([value_got, value_other], axis=3)
    key_heads = key_got.reshape(kv_local, HD, seq_len)
    value_heads = value_got.reshape(kv_local, HD, seq_len)
    attended = attention_heads(query_heads, key_heads, value_heads, seq_len)
    token_heads = lax.all_to_all(attended, "sp", split_axis=2, concat_axis=0, tiled=True)
    token_rows = token_heads.reshape(QH * HD, tok_rows)
    product = lax.dot_general(
        token_rows,
        lax.all_gather(w_out, "dp", axis=1, tiled=True),
        (((0,), (0,)), ((), ())),
        preferred_element_type=jnp.float32,
    )
    mixed_rows = product.astype(jnp.bfloat16)
    return mixed_rows[None]


MESH = pl.DeviceIdType.MESH
LOG2E = 1.4426950408889634


def layer_kernel(
    n, m, q_ref, k_ref, v_ref, qg_ref, kg_ref, cos_ref, sin_ref, w_ref, out_ref,
    q_out, k_out, q_in, k_in, v_in, a_out, a_in, w_all,
    q_send, q_recv, k_send, k_recv, v_send, v_recv, a_send, a_recv, w_send, w_recv, w_pass, w_own,
):
    me = lax.axis_index("sp")
    dp = lax.axis_index("dp")
    x_count = m // 2
    core = lax.rem(dp, 2)
    x_at = dp // 2
    partner = x_at * 2 + (1 - core)
    rows = q_ref.shape[0]
    w_rows = w_ref.shape[0] // n
    kv_width = k_out.shape[2]
    pairs = kv_width // 128
    group = q_out.shape[2] // kv_width

    def at_sp(d):
        return lax.rem(me + d, n)

    def at_dp(d):
        return lax.rem(x_at + d, x_count) * 2 + core

    barrier = pltpu.get_barrier_semaphore()

    def greet(d, carry):
        pl.semaphore_signal(barrier, inc=1, device_id={"sp": at_sp(d)}, device_id_type=MESH)
        return carry

    lax.fori_loop(1, n, greet, 0)
    for d in range(1, x_count):
        pl.semaphore_signal(barrier, inc=1, device_id={"dp": at_dp(d)}, device_id_type=MESH)
    pl.semaphore_signal(barrier, inc=1, device_id={"dp": partner}, device_id_type=MESH)
    pl.semaphore_wait(barrier, n - 1 + x_count)

    def w_piece(shard, c):
        return w_all.at[shard, pl.ds(pl.multiple_of(c * w_rows, w_rows), w_rows)]

    def w_source(c):
        return w_ref.at[pl.ds(pl.multiple_of(c * w_rows, w_rows), w_rows)]

    def w_copy(d, c):
        return pltpu.make_async_remote_copy(
            src_ref=w_source(c), dst_ref=w_piece(dp, c), send_sem=w_send.at[d, c],
            recv_sem=w_recv.at[dp, c], device_id={"dp": at_dp(d) if d else partner},
            device_id_type=MESH,
        )

    def w_came(shard, c):
        return pltpu.make_async_remote_copy(
            src_ref=w_source(c), dst_ref=w_piece(shard, c), send_sem=w_send.at[0, c],
            recv_sem=w_recv.at[shard, c], device_id={"dp": partner}, device_id_type=MESH,
        )

    def w_forward(d, c):
        shard = at_dp(d)
        return pltpu.make_async_remote_copy(
            src_ref=w_piece(shard, c), dst_ref=w_piece(shard, c), send_sem=w_pass.at[d, c],
            recv_sem=w_recv.at[shard, c], device_id={"dp": partner}, device_id_type=MESH,
        )

    def start_w(c, carry):
        for d in range(x_count):
            w_copy(d, c).start()
        return carry

    lax.fori_loop(0, n, start_w, 0)
    own_w = pltpu.make_async_copy(w_ref, w_all.at[dp], w_own)
    own_w.start()

    lane = lax.broadcasted_iota(jnp.int32, (rows, 128), 1)
    low = lane < HD
    even = (lane // (HD // 4)) % 2 == 0
    q_gain, k_gain = (jnp.concatenate([g[...], g[...]], axis=1) for g in (qg_ref, kg_ref))

    def turn(tile, gain):
        u = tile.astype(jnp.float32)
        square = u * u
        sum_low = jnp.sum(jnp.where(low, square, 0.0), axis=1, keepdims=True)
        sum_high = jnp.sum(jnp.where(low, 0.0, square), axis=1, keepdims=True)
        inverse = jnp.where(
            low, lax.rsqrt(sum_low * (1.0 / HD) + epsilon), lax.rsqrt(sum_high * (1.0 / HD) + epsilon)
        )
        normed = u * inverse * gain
        part = HD // 4
        turned = jnp.where(even, pltpu.roll(normed, 128 - part, 1), pltpu.roll(normed, part, 1))
        return normed * cos_ref[...] + turned * sin_ref[...]

    def crossed(first, second):
        one = jnp.where(low, first, pltpu.roll(second, HD, 1))
        two = jnp.where(low, pltpu.roll(first, HD, 1), second)
        return one, two

    def exchange(out, into, send, recv, d):
        peer = at_sp(d)
        return pltpu.make_async_remote_copy(
            src_ref=out.at[peer], dst_ref=into.at[me], send_sem=send.at[peer],
            recv_sem=recv.at[me], device_id={"sp": peer}, device_id_type=MESH,
        )

    def arrival(out, into, send, recv, source):
        return pltpu.make_async_remote_copy(
            src_ref=out.at[source], dst_ref=into.at[source], send_sem=send.at[source],
            recv_sem=recv.at[source], device_id={"sp": source}, device_id_type=MESH,
        )

    def kv_lanes(peer, j=0, size=kv_width):
        return pl.ds(pl.multiple_of(peer * kv_width + j * 128, 128), size)

    def turn_keys(peer, into, at):
        for j in range(pairs):
            tile = turn(k_ref[:, kv_lanes(peer, j, 128)], k_gain)
            into[at, :, j * 128 : (j + 1) * 128] = tile.astype(jnp.bfloat16)

    def turn_queries(peer, into, at):
        base = peer * (kv_width * group)
        for j in range(pairs):
            natural = [
                turn(q_ref[:, pl.ds(pl.multiple_of(base + j * 256 + i * 128, 128), 128)], q_gain)
                for i in range(2)
            ]
            for g, tile in enumerate(crossed(*natural)):
                start = g * kv_width + j * 128
                into[at, :, start : start + 128] = tile.astype(jnp.bfloat16)

    def send_values(d):
        peer = at_sp(d)
        return pltpu.make_async_remote_copy(
            src_ref=v_ref.at[:, kv_lanes(peer)], dst_ref=v_in.at[me], send_sem=v_send.at[peer],
            recv_sem=v_recv.at[me], device_id={"sp": peer}, device_id_type=MESH,
        )

    def send_kv(d, carry):
        peer = at_sp(d)
        send_values(d).start()
        turn_keys(peer, k_out, peer)
        exchange(k_out, k_in, k_send, k_recv, d).start()
        return carry

    def send_q(d, carry):
        peer = at_sp(d)
        turn_queries(peer, q_out, peer)
        exchange(q_out, q_in, q_send, q_recv, d).start()
        return carry

    lax.fori_loop(1, n, send_kv, 0)
    lax.fori_loop(1, n, send_q, 0)
    turn_keys(me, k_in, me)
    v_in[me] = v_ref[:, kv_lanes(me)]
    turn_queries(me, q_in, me)

    def await_kv(d, carry):
        source = at_sp(d)
        arrival(k_out, k_in, k_send, k_recv, source).wait_recv()
        arrival(k_out, v_in, v_send, v_recv, source).wait_recv()
        return carry

    lax.fori_loop(1, n, await_kv, 0)
    seq_len = n * rows
    scale = HD ** (-0.5) * LOG2E

    def attend(source):
        for j in range(pairs):
            keys = k_in[:, :, j * 128 : (j + 1) * 128].reshape(seq_len, 128)
            vals = v_in[:, :, j * 128 : (j + 1) * 128].reshape(seq_len, 128)
            tiles = []
            for g in range(group):
                at = g * kv_width + j * 128
                pair = q_in[source, :, at : at + 128]
                zero = jnp.zeros_like(pair)
                both = []
                for one in (jnp.where(low, pair, zero), jnp.where(low, zero, pair)):
                    s = lax.dot_general(
                        one, keys, (((1,), (1,)), ((), ())), preferred_element_type=jnp.float32
                    )
                    p = jnp.exp2((s - jnp.max(s, axis=1, keepdims=True)) * scale)
                    p = p * (1.0 / jnp.sum(p, axis=1, keepdims=True))
                    both.append(
                        jnp.dot(p.astype(jnp.bfloat16), vals, preferred_element_type=jnp.float32)
                    )
                tiles.append(jnp.where(low, both[0], both[1]))
            yield j, jnp.concatenate(crossed(*tiles), axis=1).astype(jnp.bfloat16)

    def block(d, carry):
        source = at_sp(d)
        arrival(q_out, q_in, q_send, q_recv, source).wait_recv()
        for j, tile in attend(source):
            a_out[source, :, j * 256 : (j + 1) * 256] = tile
        exchange(a_out, a_in, a_send, a_recv, d).start()
        for e in range(1, x_count):
            w_came(at_dp(e), d - 1).wait_recv()
            w_forward(e, d - 1).start()
        return carry

    lax.fori_loop(1, n, block, 0)
    for j, tile in attend(me):
        a_in[me, :, j * 256 : (j + 1) * 256] = tile
    own_w.wait()

    def came(d, carry):
        source = at_sp(d)
        arrival(a_out, a_in, a_send, a_recv, source).wait_recv()
        return carry

    lax.fori_loop(1, n, came, 0)
    width = w_ref.shape[1]

    def product(shard):
        total = jnp.zeros((rows, width), jnp.float32)
        step = a_in.shape[2]
        for p in range(n):
            total += jnp.dot(
                a_in[p], w_all[shard, p * step : (p + 1) * step, :],
                preferred_element_type=jnp.float32,
            )
        out_ref[:, pl.ds(pl.multiple_of(shard * width, width), width)] = total.astype(jnp.bfloat16)

    def await_w(shard):
        def one(c, carry):
            w_came(shard, c).wait_recv()
            return carry

        lax.fori_loop(0, n, one, 0)

    product(dp)
    await_w(partner)
    product(partner)
    for e in range(1, x_count):
        w_came(at_dp(e), n - 1).wait_recv()
        w_forward(e, n - 1).start()
    for e in range(1, x_count):
        product(at_dp(e))
    for e in range(1, x_count):
        other = at_dp(e) + 1 - 2 * core
        await_w(other)
        product(other)

    def sent(d, carry):
        exchange(k_out, k_in, k_send, k_recv, d).wait_send()
        send_values(d).wait_send()
        exchange(q_out, q_in, q_send, q_recv, d).wait_send()
        exchange(a_out, a_in, a_send, a_recv, d).wait_send()
        return carry

    lax.fori_loop(1, n, sent, 0)

    def sent_w(c, carry):
        for d in range(x_count):
            w_copy(d, c).wait_send()
        for d in range(1, x_count):
            w_forward(d, c).wait_send()
        return carry

    lax.fori_loop(0, n, sent_w, 0)


def rotary_lanes(first_row, row_count):
    position = first_row + lax.broadcasted_iota(jnp.int32, (row_count, 128), 0)
    lane = lax.broadcasted_iota(jnp.int32, (row_count, 128), 1)
    place = jnp.where(lane % HD < HD // 2, position // GRID_W, position % GRID_W)
    quarter = HD // 4
    step = (lax.iota(jnp.int32, 128) % quarter).astype(jnp.float32)
    inv_freq = rotary_base ** (-(2.0 * step) / (HD // 2))
    angle = inv_freq[None, :] * place.astype(jnp.float32)
    sign = jnp.where((lane // quarter) % 2 == 0, -1.0, 1.0)
    return (jnp.cos(angle), jnp.sin(angle) * sign)


def on_device(queries, keys, values, q_gain, k_gain, w_out):
    n, m = lax.axis_size("sp"), lax.axis_size("dp")
    tok_rows = queries.shape[2]
    kv_width = keys.shape[1] // n
    if kv_width % 128 or m % 2 or tok_rows % 16 or QH != 2 * KV:
        return on_device_plain(queries, keys, values, q_gain, k_gain, w_out)
    q_width = queries.shape[1] // n
    cos_table, sin_table = rotary_lanes(lax.axis_index("sp") * tok_rows, tok_rows)
    vmem = pl.BlockSpec(memory_space=pltpu.VMEM)
    bf16 = jnp.bfloat16
    dma = pltpu.SemaphoreType.DMA
    mixed = pl.pallas_call(
        functools.partial(layer_kernel, n, m),
        out_shape=jax.ShapeDtypeStruct((tok_rows, w_out.shape[1] * m), bf16),
        in_specs=[vmem] * 7 + [pl.BlockSpec(memory_space=pltpu.HBM)],
        out_specs=vmem,
        scratch_shapes=[
            pltpu.VMEM((n, tok_rows, q_width), bf16),
            pltpu.VMEM((n, tok_rows, kv_width), bf16),
            pltpu.VMEM((n, tok_rows, q_width), bf16),
            pltpu.VMEM((n, tok_rows, kv_width), bf16),
            pltpu.VMEM((n, tok_rows, kv_width), bf16),
            pltpu.VMEM((n, tok_rows, q_width), bf16),
            pltpu.VMEM((n, tok_rows, q_width), bf16),
            pltpu.VMEM((m, w_out.shape[0], w_out.shape[1]), bf16),
        ]
        + [dma((n,))] * 8
        + [dma((m // 2, n)), dma((m, n)), dma((m // 2, n)), dma],
        compiler_params=pltpu.CompilerParams(
            collective_id=0, has_side_effects=True, vmem_limit_bytes=48 * 1024 * 1024
        ),
    )(
        queries[0].T, keys[0].T, values[0].T, q_gain[None], k_gain[None],
        cos_table, sin_table, w_out,
    )
    return mixed[None]


def solution(mesh):
    placed = (
        P("dp", None, "sp"),
        P("dp", None, "sp"),
        P("dp", None, "sp"),
        P(),
        P(),
        P(None, "dp"),
    )
    return jax.shard_map(
        on_device, mesh=mesh, in_specs=placed, out_specs=P("dp", "sp", None), check_vma=False
    )
```
